256 devices in a mesh: fs: 16 (over y, x), tp: 16 (over z, core).
Axes of the slice: x: 4, y: 4, z: 8, core: 2. Of those that a mesh axis runs over, the one named last changes fastest.
Arguments:
- tokens: bfloat16 [16384, 2048], P(('fs', 'tp')), may hold values from -6 to 6
- gate_weight: bfloat16 [2048, 5632], P('fs', 'tp'), may hold values from -0.125 to 0.125
- up_weight: bfloat16 [2048, 5632], P('fs', 'tp'), may hold values from -0.125 to 0.125
- down_weight: bfloat16 [5632, 2048], P('tp', 'fs'), may hold values from -0.078125 to 0.078125
- grad_out: bfloat16 [16384, 2048], P(('fs', 'tp')), may hold values from -24 to 24
Outputs:
- grad_input: bfloat16 [16384, 2048], P(('fs', 'tp'))
- grad_gate: float32 [2048, 5632], P('fs', 'tp')
- grad_up: float32 [2048, 5632], P('fs', 'tp')
- grad_down: float32 [5632, 2048], P('tp', 'fs')
The draws below stay inside these ranges and needn't reach their ends.
All inputs are finite; a program needn't handle non-finite values.
Results may differ from the reference program's by a relative error of at most 0.0049.
Values may be sent and summed in bfloat16 or wider, within the bound.
A program may use at most 128 MiB of HBM per device.

```python
import jax
import jax.numpy as jnp

D = 2048
FF = 5632
TOKENS = 16384


def spiked(array, key, source, target, parts, factor):
    owner, partner = [(jnp.arange(array.shape[dim]) // (array.shape[dim] // parts)).reshape([-1 if axis == dim else 1 for axis in range(array.ndim)]) for dim in (source, target)]
    chosen = jax.random.permutation(key, parts)[partner]
    strong = (owner == chosen) | (owner == (partner + parts // 2) % parts)
    return jnp.where(strong, factor * array, array)


def shard_levels(own_key, dims, shards, least, high):
    factor_of, own = 1.0, jax.random.fold_in(own_key, 6)
    for position, shards_of in shards:
        draws = jnp.exp(jax.random.uniform(jax.random.fold_in(own, position), (shards_of,), jnp.float32, least / len(shards), high / len(shards)))
        factor_of = factor_of * jnp.repeat(draws, dims[position] // shards_of).reshape([-1 if axis == position else 1 for axis in range(len(dims))])
    return factor_of


def bell_draw(own_key, dims, spread, limit, split=(), held_as=jnp.bfloat16):
    factor_of = shard_levels(own_key, dims, split, -0.22, 0.18) if split else 1.0
    result = jax.random.normal(own_key, dims, jnp.float32) * spread * factor_of
    return jnp.minimum(jnp.maximum(result, -limit), limit).astype(held_as)


def gaussian_with(key, extent, width, bound, shards, heavy, held_as=jnp.bfloat16):
    entries = width * jax.random.normal(key, extent, jnp.float32)
    if shards:
        entries = entries * shard_levels(key, extent, shards, -0.22, 0.18)
    return jnp.clip(spiked(entries, jax.random.fold_in(key, 3), *heavy), -bound, bound).astype(held_as)


def setup_inputs(seed: int = 0) -> dict:
    splits = jax.random.split(jax.random.key(seed), 6)
    tokens = bell_draw(splits[0], (TOKENS, D), 1.0, 6.0, ((0, 256),))
    gate_weight = bell_draw(splits[1], (D, FF), D ** -0.5, 0.125, ((0, 16), (1, 16)))
    up_weight = bell_draw(splits[2], (D, FF), D ** -0.5, 0.125, ((0, 16), (1, 16)))
    down_weight = bell_draw(splits[3], (FF, D), FF ** -0.5, 0.078125, ((0, 16), (1, 16)))
    grad_out = gaussian_with(splits[4], (TOKENS, D), 1.0, 24.0, ((0, 256),), (0, 1, 256, 6.0))
    return {"tokens": tokens, "gate_weight": gate_weight, "up_weight": up_weight, "down_weight": down_weight, "grad_out": grad_out}


def reference(tokens, gate_weight, up_weight, down_weight, grad_out):
    gate_pre = jnp.dot(tokens, gate_weight, preferred_element_type=jnp.float32)
    up_pre = jnp.dot(tokens, up_weight, preferred_element_type=jnp.float32)
    sig_gate = jax.nn.sigmoid(gate_pre)
    active = gate_pre * sig_gate
    hidden = (active * up_pre).astype(jnp.bfloat16)
    d_hidden = jnp.dot(grad_out, down_weight.T, preferred_element_type=jnp.float32)
    d_gate = (d_hidden * up_pre * sig_gate * (1.0 + gate_pre * (1.0 - sig_gate))).astype(jnp.bfloat16)
    d_up = (d_hidden * active).astype(jnp.bfloat16)
    grad_input = (jnp.dot(d_gate, gate_weight.T, preferred_element_type=jnp.float32)
                  + jnp.dot(d_up, up_weight.T, preferred_element_type=jnp.float32)).astype(jnp.bfloat16)
    grad_gate = jnp.dot(tokens.T, d_gate, preferred_element_type=jnp.float32)
    grad_up = jnp.dot(tokens.T, d_up, preferred_element_type=jnp.float32)
    grad_down = jnp.dot(hidden.T, grad_out, preferred_element_type=jnp.float32)
    return grad_input, grad_gate, grad_up, grad_down
```

```python
import jax
import jax.numpy as jnp
from jax import lax
from jax.experimental import pallas as pl
from jax.experimental.pallas import tpu as pltpu
from jax.sharding import PartitionSpec as P

BF16 = jnp.bfloat16
F32 = jnp.float32
D, HID, ROWS = 2048, 352, 64
ALL = 3 * HID
NX, NY, NZ = 4, 4, 8
PAIR = 4 * ROWS
SUB = (((0, 272), (272, 528)), ((528, 800), (800, 1056)))
PLACE = {0: 0, -1: 1, 1: 2, -2: 3, 2: 4, -3: 5, 3: 6, 4: 7}
LINK_RATE, CORE_RATE, LATENCY = 46.6e3, 600e3, 2.0
GATHER = 0
SEGMENTS = 12


def slot(rel, other_core):
    return 2 * PLACE[rel] + other_core


class Task:
    def __init__(self, name, link, size, deps, copy, before=None):
        self.name, self.link, self.size, self.deps = name, link, size, deps
        self.copy, self.before = copy, before


def in_time_order(tasks, start=0.0):
    arrival, free, order, left = {}, {}, [], list(tasks)
    while left:
        best = None
        for task in left:
            if all(dep in arrival for dep in task.deps):
                ready = max([start] + [arrival[dep] for dep in task.deps])
                if best is None or ready < best[0] - 1e-9:
                    best = (ready, task)
        ready, task = best
        left.remove(task)
        order.append((ready, task))
        if task.link is None:
            arrival[task.name] = ready
        else:
            rate = CORE_RATE if task.link == "core" else LINK_RATE
            begin = max(ready, free.get(task.link, 0.0))
            free[task.link] = begin + task.size / rate
            arrival[task.name] = free[task.link] + LATENCY
    return order, arrival


def kernel(tok, gate_t, up_t, down, cot, grad_in, o_gate, o_up, o_down,
           w, xg, yg, mix, mix_t, gi, pair_in, gw,
           z_out, z_in, f_out, f_in, s_out, s_in,
           load_sem, send_sem, recv_sem):
    fs, tp = lax.axis_index("fs"), lax.axis_index("tp")
    y, x, z, core = fs // NX, fs % NX, tp // 2, tp % 2

    def device(link):
        if link == "core":
            return {"fs": fs, "tp": z * 2 + (1 - core)}
        step = 1 if link[1] == "+" else -1
        if link[0] == "z":
            return {"fs": fs, "tp": (z + NZ + step) % NZ * 2 + core}
        if link[0] == "x":
            return {"fs": y * NX + (x + NX + step) % NX, "tp": tp}
        return {"fs": (y + NY + step) % NY * NX + x, "tp": tp}

    def columns(dy, dx):
        owner = (y + NY + dy) % NY * NX + (x + NX + dx) % NX
        return pl.ds(pl.multiple_of(owner * 128, 128), 128)

    loads = [
        pltpu.make_async_copy(tok, xg.at[pl.ds(0, ROWS)], load_sem.at[0]),
        pltpu.make_async_copy(cot, yg.at[pl.ds(0, ROWS)], load_sem.at[1]),
        pltpu.make_async_copy(gate_t, w.at[pl.ds(0, HID), columns(0, 0)], load_sem.at[2]),
        pltpu.make_async_copy(up_t, w.at[pl.ds(HID, HID), columns(0, 0)], load_sem.at[3]),
        pltpu.make_async_copy(down, w.at[pl.ds(2 * HID, HID), columns(0, 0)], load_sem.at[4]),
    ]
    for load in loads:
        load.start()
    barrier = pltpu.get_barrier_semaphore()
    links = ("x+", "x-", "y+", "y-", "z+", "z-", "core")
    for link in links:
        pl.semaphore_signal(barrier, inc=1, device_id=device(link),
                            device_id_type=pl.DeviceIdType.MESH)
    pl.semaphore_wait(barrier, len(links))
    for load in loads:
        load.wait()

    number = {}

    def remote(name, link, src, dst):
        k = number.setdefault(name, len(number))
        return pltpu.make_async_remote_copy(
            src_ref=src, dst_ref=dst, send_sem=send_sem.at[k], recv_sem=recv_sem.at[k],
            device_id=device(link), device_id_type=pl.DeviceIdType.MESH)

    gather = []

    def add_tokens(name, link, ref, src, dst, deps):
        gather.append(Task(name, link, ROWS * D * 2, deps, lambda: remote(
            name, link, ref.at[pl.ds(ROWS * src, ROWS)], ref.at[pl.ds(ROWS * dst, ROWS)])))

    def add_weights(name, link, rows, dy, dx, deps):
        place = lambda: w.at[pl.ds(rows[0], rows[1] - rows[0]), columns(dy, dx)]
        gather.append(Task(name, link, (rows[1] - rows[0]) * 256, deps,
                           lambda: remote(name, link, place(), place())))

    both = (("x", xg), ("y", yg))
    for hop in range(1, 5):
        for sign, mark in ((1, "+"), (-1, "-")):
            for unit, ref in both:
                if hop == 4 and unit != ("x" if sign > 0 else "y"):
                    continue
                rel = -sign * hop if hop < 4 else 4
                add_tokens(("t", unit, rel), "z" + mark, ref, slot(-sign * (hop - 1), 0),
                           slot(rel, 0), [("t", unit, -sign * (hop - 1))] if hop > 1 else [])
    for rel in (0, -1, 1, -2, 2, -3, 3, 4):
        for unit, ref in both:
            add_tokens(("p", unit, rel), "core", ref, slot(rel, 0), slot(rel, 1),
                       [("t", unit, rel)] if rel else [])

    axes = (("x", "y"), ("y", "x"))

    def at(half, first, second):
        return (second, first) if half == 0 else (first, second)

    for stage in (1, 2):
        for half in (0, 1):
            whole = (SUB[half][0][0], SUB[half][1][1])
            axis = axes[half][stage - 1]
            for q in ((0,) if stage == 1 else (0, -1, 1, 2)):
                for sign, mark in ((1, "+"), (-1, "-")):
                    spot = (lambda r: at(half, r, 0)) if stage == 1 else (lambda r: at(half, q, r))
                    if stage == 1 or q == 0:
                        deps = []
                    elif q == 2:
                        deps = [("w", half, 1, 0, 2, 0), ("w", half, 1, 0, 2, 1)]
                    else:
                        deps = [("w", half, 1, 0, q)]
                    add_weights(("w", half, stage, q, -sign), axis + mark, whole, *spot(0), deps)
                for k, (sign, mark) in enumerate(((1, "+"), (-1, "-"))):
                    add_weights(("w", half, stage, q, 2, k), axis + mark, SUB[half][k],
                                *spot(-sign), [("w", half, stage, q, -sign)])

    order, arrival = in_time_order(gather, LATENCY)
    by_name = {task.name: task for task in gather}
    waited = set()

    def wait_for(name):
        if name not in waited:
            waited.add(name)
            by_name[name].copy().wait_recv()

    def run(tasks):
        for task in tasks:
            for dep in task.deps:
                wait_for(dep)
            if task.before is not None:
                task.before()
            if task.copy is not None:
                task.copy().start()

    gw[...] = jnp.zeros_like(gw)
    run([task for _, task in order])
    for task in sorted(gather, key=lambda t: arrival[t.name]):
        wait_for(task.name)

    def compute(p):
        rows = pl.ds(pl.multiple_of(p * PAIR, PAIR), PAIR)
        nt = (((1,), (1,)), ((), ()))
        pre = lax.dot_general(w[0:2 * HID, :], xg[rows, :], nt, preferred_element_type=F32)
        d_hidden = lax.dot_general(w[2 * HID:, :], yg[rows, :], nt, preferred_element_type=F32)
        gate, up = pre[:HID], pre[HID:]
        sig = jax.nn.sigmoid(gate)
        active = gate * sig
        mix[2 * HID:, :] = (active * up).astype(BF16)
        mix[0:HID, :] = (d_hidden * up * sig * (1.0 + gate * (1.0 - sig))).astype(BF16)
        mix[HID:2 * HID, :] = (d_hidden * active).astype(BF16)
        mix_t[...] = mix[0:2 * HID, :].T
        for n in range(0, D, 512):
            gi[rows, n:n + 512] = jnp.dot(mix_t[...], w[0:2 * HID, n:n + 512],
                                          preferred_element_type=F32)
        for n in range(0, D, 256):
            gw[0:2 * HID, n:n + 256] += jnp.dot(mix[0:2 * HID, :], xg[rows, n:n + 256],
                                                preferred_element_type=F32)
            gw[2 * HID:, n:n + 256] += jnp.dot(mix[2 * HID:, :], yg[rows, n:n + 256],
                                               preferred_element_type=F32)

    @pl.loop(0, 4)
    def _(p):
        compute(p)

    scatter = []
    half_cols = D // 2

    def add_sum(name, link, deps, make, out, into, size):
        def before():
            out()[...] = make().astype(BF16)
        scatter.append(Task(name, link, size, deps,
                            lambda: remote(name, link, out(), into()), before))

    for rel in (4, -3, 3, -2, 2, -1, 1, 0):
        def copy(rel=rel):
            return remote(("c", rel), "core", gi.at[pl.ds(ROWS * slot(rel, 1), ROWS)],
                          pair_in.at[PLACE[rel]])
        scatter.append(Task(("c", rel), "core", ROWS * D * 4, [], copy))

    def own_tokens(rel, c):
        cols = pl.ds(c * half_cols, half_cols)
        return gi[pl.ds(ROWS * slot(rel, 0), ROWS), cols] + pair_in[PLACE[rel], :, cols]

    for left in (4, 3, 2, 1):
        for k, mark in enumerate("+-"):
            for c in ((1 - k, k) if left < 4 else (k,)):
                rel = left if left == 4 or k == 0 else -left
                earlier = ("z", k, left + 1, c)
                fresh = left == 4 or (left == 3 and c != k)
                place = lambda buf, k=k, left=left, c=c: buf.at[k, left - 1, c]
                def make(rel=rel, c=c, k=k, left=left, fresh=fresh):
                    own = own_tokens(rel, c)
                    return own if fresh else own + z_in[k, left, c].astype(F32)
                add_sum(("z", k, left, c), "z" + mark,
                        [("c", rel)] + ([] if fresh else [earlier]), make,
                        lambda place=place: place(z_out), lambda place=place: place(z_in),
                        ROWS * half_cols * 2)

    def final_tokens(c):
        total = own_tokens(0, c) + z_in[0, 0, c].astype(F32) + z_in[1, 0, c].astype(F32)
        grad_in[:, pl.ds(c * half_cols, half_cols)] = total.astype(BF16)

    for c in (0, 1):
        scatter.append(Task(("zf", c), None, 0, [("c", 0), ("z", 0, 1, c), ("z", 1, 1, c)],
                            None, lambda c=c: final_tokens(c)))

    sum_axes = (("y", "x"), ("x", "y"))
    QS = {2: 0, 1: 1, -1: 2, 0: 3}

    def local(half, s):
        a, b = SUB[half][s]
        return pl.ds(a - SUB[half][0][0], b - a)

    def target(half, first, second):
        return columns(first, second) if half == 0 else columns(second, first)

    def own_grad(half, s, ra, q):
        a, b = SUB[half][s]
        return gw[pl.ds(a, b - a), target(half, ra, q)]

    def reduced(half, s, q):
        here = local(half, s)
        return (own_grad(half, s, 0, q) + f_in[half, 0, QS[q], 0, here].astype(F32)
                + f_in[half, 1, QS[q], 0, here].astype(F32))

    def reduced_deps(half, s, q):
        return [("f", half, q, 0, 1, s), ("f", half, q, 1, 1, s)]

    for kind in (0, 1, 2):
        for q in (2, 1, -1, 0):
            for half in (0, 1):
                for k, mark in enumerate("+-"):
                    sign = 1 - 2 * k
                    far, s = (2, k) if kind == 0 else (1, 1 - k if kind == 1 else k)
                    place = lambda buf, half=half, k=k, q=q, far=far, s=s: (
                        buf.at[half, k, QS[q], far - 1, local(half, s)])
                    def make(half=half, s=s, q=q, k=k, far=far, sign=sign, kind=kind):
                        own = own_grad(half, s, sign * far if far == 1 else 2, q)
                        if kind < 2:
                            return own
                        return own + f_in[half, k, QS[q], 1, local(half, s)].astype(F32)
                    add_sum(("f", half, q, k, far, s), sum_axes[half][0] + mark,
                            [("f", half, q, k, 2, s)] if kind == 2 else [], make,
                            lambda place=place: place(f_out), lambda place=place: place(f_in),
                            (SUB[half][s][1] - SUB[half][s][0]) * 256)
    for kind in (0, 1, 2):
        for half in (0, 1):
            for k, mark in enumerate("+-"):
                sign = 1 - 2 * k
                far, s = (2, k) if kind == 0 else (1, 1 - k if kind == 1 else k)
                q = 2 if far == 2 else sign
                place = lambda buf, half=half, k=k, far=far, s=s: (
                    buf.at[half, k, far - 1, local(half, s)])
                def make(half=half, s=s, q=q, k=k, kind=kind):
                    own = reduced(half, s, q)
                    if kind < 2:
                        return own
                    return own + s_in[half, k, 1, local(half, s)].astype(F32)
                add_sum(("s", half, k, far, s), sum_axes[half][1] + mark,
                        reduced_deps(half, s, q)
                        + ([("s", half, k, 2, s)] if kind == 2 else []), make,
                        lambda place=place: place(s_out), lambda place=place: place(s_in),
                        (SUB[half][s][1] - SUB[half][s][0]) * 256)

    def final_grad(half, s):
        here = local(half, s)
        total = (reduced(half, s, 0) + s_in[half, 0, 0, here].astype(F32)
                 + s_in[half, 1, 0, here].astype(F32))
        a, b = SUB[half][s]
        for m, out in enumerate((o_gate, o_up, o_down)):
            low, high = max(a, m * HID), min(b, (m + 1) * HID)
            if low < high:
                out[low - m * HID:high - m * HID, :] = total[low - a:high - a]

    for half in (0, 1):
        for s in (0, 1):
            scatter.append(Task(("sf", half, s), None, 0, reduced_deps(half, s, 0)
                                + [("s", half, k, 1, s) for k in (0, 1)],
                                None, lambda half=half, s=s: final_grad(half, s)))

    by_name.update({task.name: task for task in scatter})
    run([task for _, task in in_time_order(scatter)[0]])
    for task in gather + scatter:
        if task.copy is not None:
            wait_for(task.name) if task.name not in waited else None
            task.copy().wait_send()


COPIES = 160


def body(tokens, gate_weight, up_weight, down_weight, grad_out):
    grad = jax.ShapeDtypeStruct((HID, 128), F32)
    grad_in, g_gate, g_up, g_down = pl.pallas_call(
        kernel,
        out_shape=(jax.ShapeDtypeStruct((ROWS, D), BF16), grad, grad, grad),
        in_specs=[pl.BlockSpec(memory_space=pl.ANY)] * 5,
        out_specs=(pl.BlockSpec(memory_space=pltpu.VMEM),) * 4,
        scratch_shapes=[
            pltpu.VMEM((ALL, D), BF16),
            pltpu.VMEM((16 * ROWS, D), BF16),
            pltpu.VMEM((16 * ROWS, D), BF16),
            pltpu.VMEM((ALL, PAIR), BF16),
            pltpu.VMEM((PAIR, 2 * HID), BF16),
            pltpu.VMEM((16 * ROWS, D), F32),
            pltpu.VMEM((NZ, ROWS, D), F32),
            pltpu.VMEM((ALL, D), F32),
            pltpu.VMEM((2, 4, 2, ROWS, D // 2), BF16),
            pltpu.VMEM((2, 4, 2, ROWS, D // 2), BF16),
            pltpu.VMEM((2, 2, 4, 2, 528, 128), BF16),
            pltpu.VMEM((2, 2, 4, 2, 528, 128), BF16),
            pltpu.VMEM((2, 2, 2, 528, 128), BF16),
            pltpu.VMEM((2, 2, 2, 528, 128), BF16),
            pltpu.SemaphoreType.DMA((5,)),
            pltpu.SemaphoreType.DMA((COPIES,)),
            pltpu.SemaphoreType.DMA((COPIES,)),
        ],
        compiler_params=pltpu.CompilerParams(
            collective_id=0, has_side_effects=True, vmem_limit_bytes=66_000_000),
        name="layer",
    )(tokens, gate_weight.T, up_weight.T, down_weight, grad_out)
    return grad_in, g_gate.T, g_up.T, g_down


def solution(mesh):
    in_specs = (
        P(("fs", "tp"), None),
        P("fs", "tp"),
        P("fs", "tp"),
        P("tp", "fs"),
        P(("fs", "tp"), None),
    )
    out_specs = (P(("fs", "tp"), None), P("fs", "tp"), P("fs", "tp"), P("tp", "fs"))
    return jax.shard_map(body, mesh=mesh, in_specs=in_specs, out_specs=out_specs, check_vma=False)
```

```python
import jax
import jax.numpy as jnp
from jax import lax
from jax.experimental import pallas as pl
from jax.experimental.pallas import tpu as pltpu
from jax.sharding import PartitionSpec as P

BF16 = jnp.bfloat16
F32 = jnp.float32
D, HID, ROWS = 2048, 352, 64
ALL = 3 * HID
NX, NY, NZ = 4, 4, 8
PAIR = 4 * ROWS
SUB = (((0, 272), (272, 528)), ((528, 800), (800, 1056)))
PLACE = {0: 0, -1: 1, 1: 2, -2: 3, 2: 4, -3: 5, 3: 6, 4: 7}
LINK_RATE, CORE_RATE, LATENCY = 46.6e3, 600e3, 2.0


def slot(rel, other_core):
    return 2 * PLACE[rel] + other_core


class Task:
    def __init__(self, name, link, size, deps, copy, before=None):
        self.name, self.link, self.size, self.deps = name, link, size, deps
        self.copy, self.before = copy, before


def in_time_order(tasks, start=0.0):
    arrival, free, order, left = {}, {}, [], list(tasks)
    while left:
        best = None
        for task in left:
            if all(dep in arrival for dep in task.deps):
                ready = max([start] + [arrival[dep] for dep in task.deps])
                if best is None or ready < best[0] - 1e-9:
                    best = (ready, task)
        ready, task = best
        left.remove(task)
        order.append((ready, task))
        if task.link is None:
            arrival[task.name] = ready
        else:
            rate = CORE_RATE if task.link == "core" else LINK_RATE
            begin = max(ready, free.get(task.link, 0.0))
            free[task.link] = begin + task.size / rate
            arrival[task.name] = free[task.link] + LATENCY
    return order, arrival


def kernel(tok, gate_t, up_t, down, cot, grad_in, o_gate, o_up, o_down,
           w, xg, yg, mix, mix_t, gi, pair_in, gw,
           z_out, z_in, f_out, f_in, s_out, s_in,
           load_sem, send_sem, recv_sem):
    fs, tp = lax.axis_index("fs"), lax.axis_index("tp")
    y, x, z, core = fs // NX, fs % NX, tp // 2, tp % 2

    def device(link):
        if link == "core":
            return {"fs": fs, "tp": z * 2 + (1 - core)}
        step = 1 if link[1] == "+" else -1
        if link[0] == "z":
            return {"fs": fs, "tp": (z + NZ + step) % NZ * 2 + core}
        if link[0] == "x":
            return {"fs": y * NX + (x + NX + step) % NX, "tp": tp}
        return {"fs": (y + NY + step) % NY * NX + x, "tp": tp}

    def columns(dy, dx):
        owner = (y + NY + dy) % NY * NX + (x + NX + dx) % NX
        return pl.ds(pl.multiple_of(owner * 128, 128), 128)

    loads = [
        pltpu.make_async_copy(tok, xg.at[pl.ds(0, ROWS)], load_sem.at[0]),
        pltpu.make_async_copy(cot, yg.at[pl.ds(0, ROWS)], load_sem.at[1]),
        pltpu.make_async_copy(gate_t, w.at[pl.ds(0, HID), columns(0, 0)], load_sem.at[2]),
        pltpu.make_async_copy(up_t, w.at[pl.ds(HID, HID), columns(0, 0)], load_sem.at[3]),
        pltpu.make_async_copy(down, w.at[pl.ds(2 * HID, HID), columns(0, 0)], load_sem.at[4]),
    ]
    for load in loads:
        load.start()
    barrier = pltpu.get_barrier_semaphore()
    links = ("x+", "x-", "y+", "y-", "z+", "z-", "core")
    for link in links:
        pl.semaphore_signal(barrier, inc=1, device_id=device(link),
                            device_id_type=pl.DeviceIdType.MESH)
    pl.semaphore_wait(barrier, len(links))
    for load in loads:
        load.wait()

    number = {}

    def remote(name, link, src, dst):
        k = number.setdefault(name, len(number))
        return pltpu.make_async_remote_copy(
            src_ref=src, dst_ref=dst, send_sem=send_sem.at[k], recv_sem=recv_sem.at[k],
            device_id=device(link), device_id_type=pl.DeviceIdType.MESH)

    gather = []

    def add_tokens(name, link, ref, src, dst, deps):
        gather.append(Task(name, link, ROWS * D * 2, deps, lambda: remote(
            name, link, ref.at[pl.ds(ROWS * src, ROWS)], ref.at[pl.ds(ROWS * dst, ROWS)])))

    def add_weights(name, link, rows, dy, dx, deps):
        place = lambda: w.at[pl.ds(rows[0], rows[1] - rows[0]), columns(dy, dx)]
        gather.append(Task(name, link, (rows[1] - rows[0]) * 256, deps,
                           lambda: remote(name, link, place(), place())))

    both = (("x", xg), ("y", yg))
    for hop in range(1, 5):
        for sign, mark in ((1, "+"), (-1, "-")):
            for unit, ref in both:
                if hop == 4 and unit != ("x" if sign > 0 else "y"):
                    continue
                rel = -sign * hop if hop < 4 else 4
                add_tokens(("t", unit, rel), "z" + mark, ref, slot(-sign * (hop - 1), 0),
                           slot(rel, 0), [("t", unit, -sign * (hop - 1))] if hop > 1 else [])
    for rel in (0, -1, 1, -2, 2, -3, 3, 4):
        for unit, ref in both:
            add_tokens(("p", unit, rel), "core", ref, slot(rel, 0), slot(rel, 1),
                       [("t", unit, rel)] if rel else [])

    axes = (("x", "y"), ("y", "x"))

    def at(half, first, second):
        return (second, first) if half == 0 else (first, second)

    for stage in (1, 2):
        for half in (0, 1):
            whole = (SUB[half][0][0], SUB[half][1][1])
            axis = axes[half][stage - 1]
            for q in ((0,) if stage == 1 else (0, -1, 1, 2)):
                for sign, mark in ((1, "+"), (-1, "-")):
                    spot = (lambda r: at(half, r, 0)) if stage == 1 else (lambda r: at(half, q, r))
                    if stage == 1 or q == 0:
                        deps = []
                    elif q == 2:
                        deps = [("w", half, 1, 0, 2, 0), ("w", half, 1, 0, 2, 1)]
                    else:
                        deps = [("w", half, 1, 0, q)]
                    add_weights(("w", half, stage, q, -sign), axis + mark, whole, *spot(0), deps)
                for k, (sign, mark) in enumerate(((1, "+"), (-1, "-"))):
                    add_weights(("w", half, stage, q, 2, k), axis + mark, SUB[half][k],
                                *spot(-sign), [("w", half, stage, q, -sign)])

    order, arrival = in_time_order(gather, LATENCY)
    by_name = {task.name: task for task in gather}
    waited = set()

    def steps_of(tasks, needs=()):
        steps = []
        for task in tasks:
            for name in task.deps:
                if name not in waited:
                    waited.add(name)
                    steps.append((name, None))
            steps.append((None, task))
        for name in needs:
            if name not in waited:
                waited.add(name)
                steps.append((name, None))
        return steps

    def run(steps):
        for name, task in steps:
            if task is None:
                by_name[name].copy().wait_recv()
                continue
            if task.before is not None:
                task.before()
            if task.copy is not None:
                task.copy().start()

    gw[...] = jnp.zeros_like(gw)

    def forward(rows):
        nt = (((1,), (1,)), ((), ()))
        pre = lax.dot_general(w[0:2 * HID, :], xg[rows, :], nt, preferred_element_type=F32)
        d_hidden = lax.dot_general(w[2 * HID:, :], yg[rows, :], nt, preferred_element_type=F32)
        gate, up = pre[:HID], pre[HID:]
        sig = jax.nn.sigmoid(gate)
        active = gate * sig
        mix[2 * HID:, :] = (active * up).astype(BF16)
        mix[0:HID, :] = (d_hidden * up * sig * (1.0 + gate * (1.0 - sig))).astype(BF16)
        mix[HID:2 * HID, :] = (d_hidden * active).astype(BF16)

    def input_grad(rows):
        mix_t[...] = mix[0:2 * HID, :].T
        for n in range(0, D, 512):
            gi[rows, n:n + 512] = jnp.dot(mix_t[...], w[0:2 * HID, n:n + 512],
                                          preferred_element_type=F32)

    def weight_grad(rows):
        for n in range(0, D, 256):
            gw[0:2 * HID, n:n + 256] += jnp.dot(mix[0:2 * HID, :], xg[rows, n:n + 256],
                                                preferred_element_type=F32)
            gw[2 * HID:, n:n + 256] += jnp.dot(mix[2 * HID:, :], yg[rows, n:n + 256],
                                               preferred_element_type=F32)

    parts = ((forward, 2.0), (input_grad, 1.2), (weight_grad, 1.2))
    due, clock = {}, 0.0
    for p in range(4):
        rels = [rel for rel in PLACE if PLACE[rel] // 2 == p]
        needs = [t.name for t in gather if (t.name[0] == "w" and p == 0)
                 or (t.name[0] != "w" and t.name[2] in rels)]
        clock = max([clock] + [arrival[name] for name in needs])
        for j, (_, cost) in enumerate(parts):
            tasks = [t for ready, t in order if ready <= clock]
            order = order[len(tasks):]
            due[p, j] = steps_of(tasks, sorted(needs, key=arrival.get) if j == 0 else ())
            clock += cost
    assert not order

    @pl.loop(0, 4)
    def _(p):
        rows = pl.ds(pl.multiple_of(p * PAIR, PAIR), PAIR)
        for j, (part, _) in enumerate(parts):
            for k in range(4):
                if due[k, j]:
                    @pl.when(p == k)
                    def _():
                        run(due[k, j])
            part(rows)

    scatter = []
    half_cols = D // 2

    def add_sum(name, link, deps, make, out, into, size):
        def before():
            out()[...] = make().astype(BF16)
        scatter.append(Task(name, link, size, deps,
                            lambda: remote(name, link, out(), into()), before))

    for rel in (4, -3, 3, -2, 2, -1, 1, 0):
        def copy(rel=rel):
            return remote(("c", rel), "core", gi.at[pl.ds(ROWS * slot(rel, 1), ROWS)],
                          pair_in.at[PLACE[rel]])
        scatter.append(Task(("c", rel), "core", ROWS * D * 4, [], copy))

    def own_tokens(rel, c):
        cols = pl.ds(c * half_cols, half_cols)
        return gi[pl.ds(ROWS * slot(rel, 0), ROWS), cols] + pair_in[PLACE[rel], :, cols]

    for left in (4, 3, 2, 1):
        for k, mark in enumerate("+-"):
            for c in ((1 - k, k) if left < 4 else (k,)):
                rel = left if left == 4 or k == 0 else -left
                earlier = ("z", k, left + 1, c)
                fresh = left == 4 or (left == 3 and c != k)
                place = lambda buf, k=k, left=left, c=c: buf.at[k, left - 1, c]
                def make(rel=rel, c=c, k=k, left=left, fresh=fresh):
                    own = own_tokens(rel, c)
                    return own if fresh else own + z_in[k, left, c].astype(F32)
                add_sum(("z", k, left, c), "z" + mark,
                        [("c", rel)] + ([] if fresh else [earlier]), make,
                        lambda place=place: place(z_out), lambda place=place: place(z_in),
                        ROWS * half_cols * 2)

    def final_tokens(c):
        total = own_tokens(0, c) + z_in[0, 0, c].astype(F32) + z_in[1, 0, c].astype(F32)
        grad_in[:, pl.ds(c * half_cols, half_cols)] = total.astype(BF16)

    for c in (0, 1):
        scatter.append(Task(("zf", c), None, 0, [("c", 0), ("z", 0, 1, c), ("z", 1, 1, c)],
                            None, lambda c=c: final_tokens(c)))

    sum_axes = (("y", "x"), ("x", "y"))
    QS = {2: 0, 1: 1, -1: 2, 0: 3}

    def local(half, s):
        a, b = SUB[half][s]
        return pl.ds(a - SUB[half][0][0], b - a)

    def target(half, first, second):
        return columns(first, second) if half == 0 else columns(second, first)

    def own_grad(half, s, ra, q):
        a, b = SUB[half][s]
        return gw[pl.ds(a, b - a), target(half, ra, q)]

    def reduced(half, s, q):
        here = local(half, s)
        return (own_grad(half, s, 0, q) + f_in[half, 0, QS[q], 0, here].astype(F32)
                + f_in[half, 1, QS[q], 0, here].astype(F32))

    def reduced_deps(half, s, q):
        return [("f", half, q, 0, 1, s), ("f", half, q, 1, 1, s)]

    for kind in (0, 1, 2):
        for q in (2, 1, -1, 0):
            for half in (0, 1):
                for k, mark in enumerate("+-"):
                    sign = 1 - 2 * k
                    far, s = (2, k) if kind == 0 else (1, 1 - k if kind == 1 else k)
                    place = lambda buf, half=half, k=k, q=q, far=far, s=s: (
                        buf.at[half, k, QS[q], far - 1, local(half, s)])
                    def make(half=half, s=s, q=q, k=k, far=far, sign=sign, kind=kind):
                        own = own_grad(half, s, sign * far if far == 1 else 2, q)
                        if kind < 2:
                            return own
                        return own + f_in[half, k, QS[q], 1, local(half, s)].astype(F32)
                    add_sum(("f", half, q, k, far, s), sum_axes[half][0] + mark,
                            [("f", half, q, k, 2, s)] if kind == 2 else [], make,
                            lambda place=place: place(f_out), lambda place=place: place(f_in),
                            (SUB[half][s][1] - SUB[half][s][0]) * 256)
    for kind in (0, 1, 2):
        for half in (0, 1):
            for k, mark in enumerate("+-"):
                sign = 1 - 2 * k
                far, s = (2, k) if kind == 0 else (1, 1 - k if kind == 1 else k)
                q = 2 if far == 2 else sign
                place = lambda buf, half=half, k=k, far=far, s=s: (
                    buf.at[half, k, far - 1, local(half, s)])
                def make(half=half, s=s, q=q, k=k, kind=kind):
                    own = reduced(half, s, q)
                    if kind < 2:
                        return own
                    return own + s_in[half, k, 1, local(half, s)].astype(F32)
                add_sum(("s", half, k, far, s), sum_axes[half][1] + mark,
                        reduced_deps(half, s, q)
                        + ([("s", half, k, 2, s)] if kind == 2 else []), make,
                        lambda place=place: place(s_out), lambda place=place: place(s_in),
                        (SUB[half][s][1] - SUB[half][s][0]) * 256)

    def final_grad(half, s):
        here = local(half, s)
        total = (reduced(half, s, 0) + s_in[half, 0, 0, here].astype(F32)
                 + s_in[half, 1, 0, here].astype(F32))
        a, b = SUB[half][s]
        for m, out in enumerate((o_gate, o_up, o_down)):
            low, high = max(a, m * HID), min(b, (m + 1) * HID)
            if low < high:
                out[low - m * HID:high - m * HID, :] = total[low - a:high - a]

    for half in (0, 1):
        for s in (0, 1):
            scatter.append(Task(("sf", half, s), None, 0, reduced_deps(half, s, 0)
                                + [("s", half, k, 1, s) for k in (0, 1)],
                                None, lambda half=half, s=s: final_grad(half, s)))

    by_name.update({task.name: task for task in scatter})
    run(steps_of([task for _, task in in_time_order(scatter)[0]]))
    for task in gather + scatter:
        if task.copy is not None:
            task.copy().wait_send()


COPIES = 160


def write_out(*refs):
    sources, results, sem = refs[:4], refs[4:8], refs[8]
    copies = [pltpu.make_async_copy(a, b, sem.at[k])
              for k, (a, b) in enumerate(zip(sources, results))]
    for copy in copies:
        copy.start()
    for copy in copies:
        copy.wait()


def body(tokens, gate_weight, up_weight, down_weight, grad_out):
    grad = jax.ShapeDtypeStruct((HID, 128), F32)
    shapes = (jax.ShapeDtypeStruct((ROWS, D), BF16), grad, grad, grad)
    sums = pl.pallas_call(
        kernel,
        out_shape=shapes,
        in_specs=[pl.BlockSpec(memory_space=pltpu.HBM)] * 5,
        out_specs=(pl.BlockSpec(memory_space=pltpu.VMEM),) * 4,
        scratch_shapes=[
            pltpu.VMEM((ALL, D), BF16),
            pltpu.VMEM((16 * ROWS, D), BF16),
            pltpu.VMEM((16 * ROWS, D), BF16),
            pltpu.VMEM((ALL, PAIR), BF16),
            pltpu.VMEM((PAIR, 2 * HID), BF16),
            pltpu.VMEM((16 * ROWS, D), F32),
            pltpu.VMEM((NZ, ROWS, D), F32),
            pltpu.VMEM((ALL, D), F32),
            pltpu.VMEM((2, 4, 2, ROWS, D // 2), BF16),
            pltpu.VMEM((2, 4, 2, ROWS, D // 2), BF16),
            pltpu.VMEM((2, 2, 4, 2, 528, 128), BF16),
            pltpu.VMEM((2, 2, 4, 2, 528, 128), BF16),
            pltpu.VMEM((2, 2, 2, 528, 128), BF16),
            pltpu.VMEM((2, 2, 2, 528, 128), BF16),
            pltpu.SemaphoreType.DMA((5,)),
            pltpu.SemaphoreType.DMA((COPIES,)),
            pltpu.SemaphoreType.DMA((COPIES,)),
        ],
        compiler_params=pltpu.CompilerParams(
            collective_id=0, has_side_effects=True, vmem_limit_bytes=54_000_000),
        name="layer",
    )(*(pltpu.with_memory_space_constraint(v, pltpu.HBM)
        for v in (tokens, gate_weight.T, up_weight.T, down_weight, grad_out)))
    grad_in, g_gate, g_up, g_down = pl.pallas_call(
        write_out,
        out_shape=shapes,
        in_specs=[pl.BlockSpec(memory_space=pltpu.VMEM)] * 4,
        out_specs=(pl.BlockSpec(memory_space=pltpu.HBM),) * 4,
        scratch_shapes=[pltpu.SemaphoreType.DMA((4,))],
        compiler_params=pltpu.CompilerParams(vmem_limit_bytes=4_000_000),
        name="write_out",
    )(*sums)
    return grad_in, g_gate.T, g_up.T, g_down


def solution(mesh):
    in_specs = (
        P(("fs", "tp"), None),
        P("fs", "tp"),
        P("fs", "tp"),
        P("tp", "fs"),
        P(("fs", "tp"), None),
    )
    out_specs = (P(("fs", "tp"), None), P("fs", "tp"), P("fs", "tp"), P("tp", "fs"))
    return jax.shard_map(body, mesh=mesh, in_specs=in_specs, out_specs=out_specs, check_vma=False)
```
